256 devices in a mesh: ep: 32 (over z, x), tp: 8 (over y, core).
Axes of the slice: x: 4, y: 4, z: 8, core: 2. Of those that a mesh axis runs over, the one named last changes fastest.
Arguments:
- tokens: bfloat16 [512, 2048], P('ep'), may hold values from -6 to 6
- lengths: int32 [512], P('ep'), may hold values from 1024 to 16384
- old_state: float32 [512, 8, 128, 128], P('ep', 'tp'), may hold values from -2 to 2
- query_weight: bfloat16 [2048, 1024], P(None, 'tp'), may hold values from -0.125 to 0.125
- key_weight: bfloat16 [2048, 1024], P(None, 'tp'), may hold values from -0.125 to 0.125
- value_weight: bfloat16 [2048, 1024], P(None, 'tp'), may hold values from -0.125 to 0.125
- gate_weight: bfloat16 [2048, 1024], P(None, 'tp'), may hold values from -0.125 to 0.125
- head_gain: float32 [1024], P('tp'), may hold values from 0.1 to 1.9
- output_weight: bfloat16 [1024, 2048], P('tp'), may hold values from -0.1875 to 0.1875
- first_gain: float32 [2048], replicated, may hold values from 0.1 to 1.9
- expert_ids: int32 [512, 6], P('ep'), may hold values from 0 to 63, all different within a row; in each aligned block of 16 rows (0 to 15, 16 to 31, ...) at most 2 rows name the same one
- expert_weights: float32 [512, 6], P('ep'), may hold values from 0.05 to 0.8
- expert_gate: bfloat16 [64, 2048, 512], P('ep', None, 'tp'), may hold values from -0.125 to 0.125
- expert_up: bfloat16 [64, 2048, 512], P('ep', None, 'tp'), may hold values from -0.125 to 0.125
- expert_down: bfloat16 [64, 512, 2048], P('ep', 'tp'), may hold values from -0.25 to 0.25
- shared_gate: bfloat16 [2048, 512], P(None, 'tp'), may hold values from -0.125 to 0.125
- shared_up: bfloat16 [2048, 512], P(None, 'tp'), may hold values from -0.125 to 0.125
- shared_down: bfloat16 [512, 2048], P('tp'), may hold values from -0.25 to 0.25
- side_gate: bfloat16 [2048], replicated, may hold values from -0.125 to 0.125
- dense_gate: bfloat16 [2048, 8192], P(None, ('ep', 'tp')), may hold values from -0.125 to 0.125
- dense_up: bfloat16 [2048, 8192], P(None, ('ep', 'tp')), may hold values from -0.125 to 0.125
- dense_down: bfloat16 [8192, 2048], P(('ep', 'tp')), may hold values from -0.25 to 0.25
- second_gain: float32 [2048], replicated, may hold values from 0.1 to 1.9
Outputs:
- layer_out: bfloat16 [512, 2048], P('ep')
- new_state: float32 [512, 8, 128, 128], P('ep', 'tp')
The draws below stay inside these ranges and needn't reach their ends.
Inputs may be any that keep to these rules, and one draw needn't show every extreme that they name: `expert_ids`: each row names 6 different experts. Among the 16 rows of one index of ep no expert is named by more than 2 rows, a bound that some block reaches.
All inputs are finite; a program needn't handle non-finite values.
Results may differ from the reference program's by a relative error of at most 0.017.
Values may be sent and summed in bfloat16 or wider, within the bound.
No kernel may reach another device: no remote copies, remote signals or barrier semaphores. Data moves between devices by JAX's collectives and lax.ppermute only.
A program may use at most 64 MiB of HBM per device.

```python
import math
import jax
import jax.numpy as jnp
import numpy as np
from jax import lax

D = 2048
HEADS = 8
HD = 128
EFF = 512
SFF = 512
DENSE_FF = 8192
TOPK = 6
SEQ_DEV = 16
EXPERTS = 64
TOKENS = 512
CAP = 2
N_EP = 32
N_TP = 8


def set_ends(array, stream_key, low, high):
    extent = array.shape
    spot = [jax.random.randint(jax.random.fold_in(stream_key, axis), (), 0, extent[axis]) for axis in range(len(extent))]
    array = array.at[tuple(spot)].set(low)
    longest = extent.index(max(extent))
    spot[longest] = (spot[longest] + 1) % extent[longest]
    return array.at[tuple(spot)].set(high)


def levels(rng, extent, cuts, low, largest):
    gain, own = 1.0, jax.random.fold_in(rng, 6)
    for dim, parts in cuts:
        draws = jnp.exp(jax.random.uniform(jax.random.fold_in(own, dim), (parts,), jnp.float32, low / len(cuts), largest / len(cuts)))
        gain = gain * jnp.repeat(draws, extent[dim] // parts).reshape([-1 if axis == dim else 1 for axis in range(len(extent))])
    return gain


def deal_out(own_key, own, number, rows, amount, top, reach, lean):
    ranking = jax.random.permutation(own_key, amount)
    crowded, ordinary = shares(amount, rows * top, reach, lean, True), shares(amount, rows * top, reach, lean, False)
    places = jnp.arange(amount)

    def named(sizes, turn):
        used = int((sizes > 0).sum())
        fixed = max(1, used // 4)
        moved = fixed + (places - fixed + turn * (used - fixed)) % max(1, amount - fixed)
        return jnp.zeros((amount,), jnp.int32).at[ranking[jnp.where(places < fixed, places, moved)]].set(jnp.asarray(sizes, jnp.int32))

    sizes = jnp.where(number % 4 == 0, named(crowded, number // 4), named(ordinary, number - number // 4 - 1))
    mixed = jax.random.permutation(jax.random.fold_in(own, 3), amount)
    donor, receiver = mixed[0:amount // 2 * 2:2], mixed[1:amount // 2 * 2:2]
    margin = jnp.minimum(sizes[donor] - 1, reach - sizes[receiver]) // 2
    margin = jnp.where((donor == ranking[0]) | (receiver == ranking[0]) | (sizes[receiver] == 0), 0, jnp.maximum(margin, 0))
    moved = jax.random.randint(jax.random.fold_in(own, 4), (amount // 2,), 0, 1 << 20) % (margin + 1)
    sizes = sizes.at[donor].add(-moved).at[receiver].add(moved)
    items = jnp.searchsorted(jnp.cumsum(sizes), jnp.arange(rows * top), side="right").astype(jnp.int32)
    listing = items.reshape(top, rows).T
    listing = listing[jax.random.permutation(jax.random.fold_in(own, 1), rows)]
    turn = jax.random.randint(jax.random.fold_in(own, 2), (rows, 1), 0, top)
    return jnp.take_along_axis(listing, (jnp.arange(top)[None, :] + turn) % top, axis=1)


def shares(number_of, total, limit, lean, full):
    weights = [(1 << 20) // math.isqrt(standing ** lean) + 1 for standing in range(1, number_of + 1)]
    largest = limit if full else min(limit, max(-(-total // number_of), total * weights[0] // sum(weights)))
    least = 1 if total - largest >= number_of - 1 else 0
    counts, spare = [largest] + [least] * (number_of - 1), total - largest - least * (number_of - 1)
    while spare > 0:
        free = [i for i in range(1, number_of) if counts[i] < largest] or [i for i in range(1, number_of) if counts[i] < limit]
        pool, left = sum([weights[i] for i in free]), spare
        for i in free:
            extra = min(limit - counts[i], max(1, left * weights[i] // pool), spare)
            counts[i] = counts[i] + extra
            spare = spare - extra
    return np.array(counts)


def scatter_about(key, dims, width, limit, shards=(), held_as=jnp.bfloat16):
    factor_of = levels(key, dims, shards, -0.22, 0.18) if shards else 1.0
    drawn = jax.random.normal(key, dims, jnp.float32) * width * factor_of
    return jnp.minimum(jnp.maximum(drawn, -limit), limit).astype(held_as)


def setup_inputs(seed: int = 0) -> dict:
    key_of = jax.random.split(jax.random.key(seed), 24)
    tokens = scatter_about(key_of[0], (TOKENS, D), 1.0, 6.0, ((0, 32),))
    lengths = set_ends(jax.random.randint(key_of[1], (TOKENS,), 1024, 16385), jax.random.fold_in(key_of[1], 1), 1024, 16384).astype(jnp.int32)
    old_state = scatter_about(key_of[2], (TOKENS, HEADS, HD, HD), 0.25, 2.0, ((0, 32), (1, 8)), jnp.float32)
    query_weight = scatter_about(key_of[3], (D, HEADS * HD), D ** -0.5, 0.125, ((1, 8),))
    key_weight = scatter_about(key_of[4], (D, HEADS * HD), D ** -0.5, 0.125, ((1, 8),))
    value_weight = scatter_about(key_of[5], (D, HEADS * HD), D ** -0.5, 0.125, ((1, 8),))
    gate_weight = scatter_about(key_of[6], (D, HEADS * HD), D ** -0.5, 0.125, ((1, 8),))
    head_gain = jnp.clip(1.0 + 0.18 * jax.random.normal(key_of[7], (HEADS * HD,), jnp.float32), 0.1, 1.9)
    output_weight = scatter_about(key_of[8], (HEADS * HD, D), (HEADS * HD) ** -0.5, 0.1875, ((0, 8),))
    first_gain = jnp.clip(1.0 + 0.18 * jax.random.normal(key_of[9], (D,), jnp.float32), 0.1, 1.9)
    expert_ids_keys = jax.random.split(jax.random.fold_in(key_of[10], 1), TOKENS // SEQ_DEV)
    expert_ids_turns = jax.random.permutation(jax.random.fold_in(key_of[10], 3), TOKENS // SEQ_DEV)
    expert_ids = jax.vmap(lambda own, number: deal_out(jax.random.fold_in(key_of[10], 2), own, number, SEQ_DEV, EXPERTS, TOPK, CAP, 2))(expert_ids_keys, expert_ids_turns).reshape((TOKENS, TOPK))
    expert_weights = jnp.clip(jnp.exp(math.log(0.8) - 2.7725887 * jax.random.uniform(key_of[11], (TOKENS, TOPK), jnp.float32) ** levels(key_of[11], (TOKENS, TOPK), ((0, 32),), -0.2, 0.2)), 0.05, 0.8)
    expert_gate = scatter_about(key_of[12], (EXPERTS, D, EFF), D ** -0.5, 0.125, ((0, 32), (2, 8)))
    expert_up = scatter_about(key_of[13], (EXPERTS, D, EFF), D ** -0.5, 0.125, ((0, 32), (2, 8)))
    expert_down = scatter_about(key_of[14], (EXPERTS, EFF, D), EFF ** -0.5, 0.25, ((0, 32), (1, 8)))
    shared_gate = scatter_about(key_of[15], (D, SFF), D ** -0.5, 0.125, ((1, 8),))
    shared_up = scatter_about(key_of[16], (D, SFF), D ** -0.5, 0.125, ((1, 8),))
    shared_down = scatter_about(key_of[17], (SFF, D), SFF ** -0.5, 0.25, ((0, 8),))
    side_gate = scatter_about(key_of[18], (D,), D ** -0.5, 0.125)
    dense_gate = scatter_about(key_of[19], (D, DENSE_FF), D ** -0.5, 0.125, ((1, 256),))
    dense_up = scatter_about(key_of[20], (D, DENSE_FF), D ** -0.5, 0.125, ((1, 256),))
    dense_down = scatter_about(key_of[21], (DENSE_FF, D), (DENSE_FF // 16) ** -0.5, 0.25, ((0, 256),))
    second_gain = jnp.clip(1.0 + 0.18 * jax.random.normal(key_of[22], (D,), jnp.float32), 0.1, 1.9)
    return {"tokens": tokens, "lengths": lengths, "old_state": old_state, "query_weight": query_weight, "key_weight": key_weight, "value_weight": value_weight, "gate_weight": gate_weight, "head_gain": head_gain, "output_weight": output_weight, "first_gain": first_gain, "expert_ids": expert_ids, "expert_weights": expert_weights, "expert_gate": expert_gate, "expert_up": expert_up, "expert_down": expert_down, "shared_gate": shared_gate, "shared_up": shared_up, "shared_down": shared_down, "side_gate": side_gate, "dense_gate": dense_gate, "dense_up": dense_up, "dense_down": dense_down, "second_gain": second_gain}


NORM_EPS = 1e-05
RESIDUAL_SCALE = 2.0 ** 0.5

def rotate(inputs, positions):
    half_size = inputs.shape[-1] // 2
    frequency = 1.0 / 10000.0 ** (jnp.arange(half_size, dtype=jnp.float32) * 2.0 / inputs.shape[-1])
    angles = positions.astype(jnp.float32)[:, None] * frequency[None, :]
    cosine = jnp.cos(angles)[:, None, :]
    sine_part = jnp.sin(angles)[:, None, :]
    first_half = inputs[..., :half_size]
    second_half = inputs[..., half_size:]
    return jnp.concatenate([first_half * cosine - second_half * sine_part, first_half * sine_part + second_half * cosine], axis=-1)

def layer_norm(inputs, scale_gain):
    average = lax.optimization_barrier(jnp.mean(inputs, axis=-1, keepdims=True))
    centered = inputs - average
    variance = lax.optimization_barrier(jnp.mean(centered * centered, axis=-1, keepdims=True))
    return centered * lax.rsqrt(variance + NORM_EPS) * scale_gain

def reference(tokens, lengths, old_state, query_weight, key_weight, value_weight, gate_weight, head_gain, output_weight, first_gain, expert_ids, expert_weights, expert_gate, expert_up, expert_down, shared_gate, shared_up, shared_down, side_gate, dense_gate, dense_up, dense_down, second_gain):
    row_count = tokens.shape[0]
    head_count = old_state.shape[1]
    head_size = old_state.shape[-1]
    model_width = tokens.shape[1]
    queries = jnp.dot(tokens, query_weight, preferred_element_type=jnp.float32).reshape(row_count, head_count, head_size)
    keys_raw = jnp.dot(tokens, key_weight, preferred_element_type=jnp.float32).reshape(row_count, head_count, head_size)
    keys_raw = keys_raw * head_size ** (-0.5)
    values = jnp.dot(tokens, value_weight, preferred_element_type=jnp.float32).reshape(row_count, head_count, head_size)
    gating = jnp.dot(tokens, gate_weight, preferred_element_type=jnp.float32)
    query_rot = rotate(queries, lengths)
    key_rot = rotate(keys_raw, lengths)
    head_ids = jnp.arange(head_count, dtype=jnp.float32)
    decays = 1.0 - jnp.exp2(-2.0 - 10.0 * head_ids / (HEADS - 1))
    new_state = decays[None, :, None, None] * old_state + key_rot[:, :, :, None] * values[:, :, None, :]
    readout = jnp.einsum('thi,thij->thj', query_rot, new_state, precision=lax.Precision.HIGHEST)
    normed = layer_norm(readout, head_gain.reshape(head_count, head_size))
    mixed = (normed.reshape(row_count, head_count * head_size) * jax.nn.silu(gating)).astype(jnp.bfloat16)
    group_width = head_count * head_size // N_TP
    branch = jnp.zeros((row_count, model_width), jnp.float32)
    for shard_index in range(N_TP):
        lower = shard_index * group_width
        product = jnp.dot(mixed[:, lower:lower + group_width], output_weight[lower:lower + group_width], preferred_element_type=jnp.float32).astype(jnp.bfloat16)
        branch = branch + lax.optimization_barrier(product).astype(jnp.float32)
    after_mixer = layer_norm(RESIDUAL_SCALE * tokens.astype(jnp.float32) + branch, first_gain).astype(jnp.bfloat16)
    top_count = expert_ids.shape[1]
    expert_count = expert_gate.shape[0]
    slot_total = N_EP * CAP
    flat_ids = expert_ids.reshape(-1).astype(jnp.int32)
    pair_count = flat_ids.shape[0]
    onehot = (flat_ids[:, None] == jnp.arange(expert_count, dtype=jnp.int32)[None, :]).astype(jnp.int32)
    slot_rank = lax.optimization_barrier(jnp.sum(onehot * (jnp.cumsum(onehot, axis=0) - 1), axis=1))
    targets = (flat_ids * slot_total + slot_rank).astype(jnp.int32)
    owners = (jnp.arange(pair_count, dtype=jnp.int32) // top_count).astype(jnp.int32)
    table = jnp.zeros((expert_count * slot_total,), jnp.int32).at[targets].set(owners)
    gathered = after_mixer[table].reshape(expert_count, slot_total, model_width)
    hidden_width = expert_gate.shape[2] // N_TP

    def one_expert(operands):
        rows_in, gate_mat, up_mat, down_mat = operands
        gate_part = jnp.dot(rows_in, gate_mat, preferred_element_type=jnp.float32)
        up_part = jnp.dot(rows_in, up_mat, preferred_element_type=jnp.float32)
        hidden = (jax.nn.silu(gate_part) * up_part).astype(jnp.bfloat16)
        summed = jnp.zeros((rows_in.shape[0], model_width), jnp.float32)
        for shard_index in range(N_TP):
            lower = shard_index * hidden_width
            product = jnp.dot(hidden[:, lower:lower + hidden_width], down_mat[lower:lower + hidden_width], preferred_element_type=jnp.float32).astype(jnp.bfloat16)
            summed = summed + lax.optimization_barrier(product).astype(jnp.float32)
        return summed.astype(jnp.bfloat16)
    outputs = lax.map(one_expert, (gathered, expert_gate, expert_up, expert_down))
    picked = outputs.reshape(expert_count * slot_total, model_width)[targets].astype(jnp.float32)
    picked = picked.reshape(row_count, top_count, model_width)
    routed = lax.optimization_barrier(jnp.sum(picked * expert_weights[:, :, None], axis=1))
    switch = jax.nn.sigmoid(jnp.dot(after_mixer, side_gate, preferred_element_type=jnp.float32))
    dense_hidden = (jax.nn.silu(jnp.dot(after_mixer, dense_gate, preferred_element_type=jnp.float32)) * jnp.dot(after_mixer, dense_up, preferred_element_type=jnp.float32) * switch[:, None]).astype(jnp.bfloat16)
    shared_hidden = (jax.nn.silu(jnp.dot(after_mixer, shared_gate, preferred_element_type=jnp.float32)) * jnp.dot(after_mixer, shared_up, preferred_element_type=jnp.float32)).astype(jnp.bfloat16)
    side = (jnp.dot(dense_hidden, dense_down, preferred_element_type=jnp.float32) + jnp.dot(shared_hidden, shared_down, preferred_element_type=jnp.float32)).astype(jnp.bfloat16)
    total = RESIDUAL_SCALE * after_mixer.astype(jnp.float32) + routed + side.astype(jnp.float32)
    layer_out = layer_norm(total, second_gain).astype(jnp.bfloat16)
    return (layer_out, new_state)
```

```python
import jax
import jax.numpy as jnp
from jax import lax
from jax.sharding import Mesh
from jax.sharding import PartitionSpec as P

HEADS = 8
EP = ("z", "x")
TP = ("y", "c")
ALL = ("z", "x", "y", "c")
NORM_EPS = 1e-05
RESIDUAL_SCALE = 2.0**0.5
BF = jnp.bfloat16
F32 = jnp.float32


def shifted(value, axis, step):
    n = lax.axis_size(axis)
    return lax.ppermute(value, axis, [(i, (i + step) % n) for i in range(n)])


def rotate(inputs, positions):
    half = inputs.shape[-1] // 2
    frequency = 1.0 / 10000.0 ** (jnp.arange(half, dtype=F32) * 2.0 / inputs.shape[-1])
    angles = positions.astype(F32)[:, None] * frequency[None, :]
    cosine = jnp.cos(angles)[:, None, :]
    sine = jnp.sin(angles)[:, None, :]
    first = inputs[..., :half]
    second = inputs[..., half:]
    return jnp.concatenate(
        [first * cosine - second * sine, first * sine + second * cosine], axis=-1
    )


def layer_norm(inputs, gain):
    average = jnp.mean(inputs, axis=-1, keepdims=True)
    centered = inputs - average
    variance = jnp.mean(centered * centered, axis=-1, keepdims=True)
    return centered * lax.rsqrt(variance + NORM_EPS) * gain


def per_device(
    tokens,
    lengths,
    old_state,
    query_weight,
    key_weight,
    value_weight,
    gate_weight,
    head_gain,
    output_weight,
    first_gain,
    expert_ids,
    expert_weights,
    expert_gate,
    expert_up,
    expert_down,
    shared_gate,
    shared_up,
    shared_down,
    side_gate,
    dense_gate,
    dense_up,
    dense_down,
    second_gain,
):
    rows, width = tokens.shape
    half = rows // 2
    local_heads, head_size = old_state.shape[1], old_state.shape[-1]
    nz, nx, ny, nc = (lax.axis_size(a) for a in ALL)
    zi, xi, yi, ci = (lax.axis_index(a) for a in ALL)
    top = expert_ids.shape[1]

    def project(weight):
        return jnp.dot(tokens, weight, preferred_element_type=F32).reshape(
            rows, local_heads, head_size
        )

    queries = project(query_weight)
    keys = project(key_weight) * head_size ** (-0.5)
    values = project(value_weight)
    gating = jnp.dot(tokens, gate_weight, preferred_element_type=F32)
    query_rot = rotate(queries, lengths)
    key_rot = rotate(keys, lengths)
    head_ids = (
        (yi * nc + ci) * local_heads + jnp.arange(local_heads, dtype=jnp.int32)
    ).astype(F32)
    decays = 1.0 - jnp.exp2(-2.0 - 10.0 * head_ids / (HEADS - 1))
    new_state = (
        decays[None, :, None, None] * old_state
        + key_rot[:, :, :, None] * values[:, :, None, :]
    )
    readout = jnp.einsum(
        "thi,thij->thj", query_rot, new_state, precision=lax.Precision.HIGHEST
    )
    normed = layer_norm(readout, head_gain.reshape(local_heads, head_size))
    mixed = (normed.reshape(rows, -1) * jax.nn.silu(gating)).astype(BF)
    partial = jnp.dot(mixed, output_weight, preferred_element_type=F32).astype(BF)

    halves = partial.reshape(2, half, width)
    kept = lax.dynamic_index_in_dim(halves, ci, 0, False)
    given = lax.dynamic_index_in_dim(halves, 1 - ci, 0, False)
    pair = (kept.astype(F32) + shifted(given, "c", 1).astype(F32)).astype(BF)

    packed_in, packed_out = lax.optimization_barrier(
        (
            (expert_gate, expert_up, dense_gate, dense_up, shared_gate, shared_up,
             expert_down, dense_down, shared_down),
            pair,
        )
    )
    pair = packed_out
    eg, eu, dg, du, sg, su, ed, dd, sd = packed_in
    experts = eg.shape[0]
    eff, dff, sff = eg.shape[2], dg.shape[1], sg.shape[1]
    wg = jnp.concatenate([eg[e] for e in range(experts)] + [dg, sg], axis=1)
    wu = jnp.concatenate([eu[e] for e in range(experts)] + [du, su], axis=1)
    w_own = jnp.stack([wg, wu])
    d_own = jnp.concatenate([ed.reshape(-1, width), dd, sd], axis=0)

    branch = pair.astype(F32)
    for k in range(1, ny):
        branch = branch + shifted(pair, "y", k).astype(F32)
    w_peer = shifted(w_own, "c", 1)
    d_peer = shifted(d_own, "c", 1)
    my_tokens = lax.dynamic_index_in_dim(tokens.reshape(2, half, width), ci, 0, False)
    after = layer_norm(RESIDUAL_SCALE * my_tokens.astype(F32) + branch, first_gain).astype(BF)

    my_ids = lax.dynamic_index_in_dim(expert_ids.reshape(2, half, top), ci, 0, False)
    my_w = lax.dynamic_index_in_dim(expert_weights.reshape(2, half, top), ci, 0, False)
    w_high = my_w.astype(BF)
    w_low = (my_w - w_high.astype(F32)).astype(BF)
    info = jnp.concatenate(
        [my_ids.astype(BF), w_high, w_low, jnp.zeros((half, 128 - 3 * top), BF)], axis=1
    )
    sent = jnp.concatenate([after, info], axis=1)
    span = sent.shape[1]
    block = lax.all_to_all(
        jnp.broadcast_to(sent[None], (nz, half, span)), "z", 0, 0, tiled=True
    ).reshape(nz * half, span)
    blocks = [block] + [shifted(block, "x", k) for k in range(1, nx)]
    every = jnp.concatenate(blocks, axis=0)
    acts = every[:, :width]
    ids = every[:, width : width + top].astype(jnp.int32)
    weights = every[:, width + top : width + 2 * top].astype(F32) + every[
        :, width + 2 * top : width + 3 * top
    ].astype(F32)

    total = every.shape[0]
    first_expert = (zi * nx + xi) * experts
    switch = jax.nn.sigmoid(jnp.dot(acts, side_gate, preferred_element_type=F32))
    scales = []
    for e in range(experts):
        share = jnp.sum(jnp.where(ids == first_expert + e, weights, 0.0), axis=1)
        scales.append(jnp.broadcast_to(share[:, None], (total, eff)))
    row = jnp.arange(total, dtype=jnp.int32)
    own = jnp.logical_and(row >= zi * half, row < (zi + 1) * half).astype(F32)
    scales.append(jnp.broadcast_to(switch[:, None], (total, dff)))
    scales.append(jnp.broadcast_to(own[:, None], (total, sff)))
    scale = jnp.concatenate(scales, axis=1)

    def hidden_of(w):
        gate = jnp.dot(acts, w[0], preferred_element_type=F32)
        up = jnp.dot(acts, w[1], preferred_element_type=F32)
        return (jax.nn.silu(gate) * up * scale).astype(BF)

    h_own = hidden_of(w_own)
    h_peer = hidden_of(w_peer)

    piece = width // ny
    reduced = None
    for k in range(ny - 1, -1, -1):
        start = ((yi + k) % ny) * piece
        part = jnp.dot(
            h_own, lax.dynamic_slice_in_dim(d_own, start, piece, 1), preferred_element_type=F32
        ) + jnp.dot(
            h_peer, lax.dynamic_slice_in_dim(d_peer, start, piece, 1), preferred_element_type=F32
        )
        if k:
            part = shifted(part.astype(BF), "y", k).astype(F32)
        reduced = part if reduced is None else reduced + part

    per_x = nz * half
    summed = reduced[:per_x]
    for k in range(1, nx):
        summed = summed + shifted(
            reduced[k * per_x : (k + 1) * per_x].astype(BF), "x", nx - k
        ).astype(F32)
    back = lax.all_to_all(
        summed.astype(BF).reshape(nz, half, piece), "z", 0, 0, tiled=True
    )
    mine = jnp.sum(back.astype(F32), axis=0)

    canvas = jnp.zeros((ny, half, piece), F32)
    for k in range(ny):
        got = shifted(mine, "y", k) if k else mine
        canvas = lax.dynamic_update_index_in_dim(canvas, got, (yi - k) % ny, 0)
    branch_sum = jnp.moveaxis(canvas, 0, 1).reshape(half, width)
    final = layer_norm(RESIDUAL_SCALE * after.astype(F32) + branch_sum, second_gain).astype(BF)
    other = shifted(final, "c", 1)
    low = jnp.where(ci == 0, final, other)
    high = jnp.where(ci == 0, other, final)
    layer_out = jnp.concatenate([low, high], axis=0)
    return (layer_out, new_state)


def solution(mesh):
    finer = Mesh(mesh.devices.reshape(8, 4, 4, 2), ALL)
    return jax.shard_map(
        per_device,
        mesh=finer,
        in_specs=(
            P(EP, None),
            P(EP),
            P(EP, TP, None, None),
            P(None, TP),
            P(None, TP),
            P(None, TP),
            P(None, TP),
            P(TP),
            P(TP, None),
            P(),
            P(EP, None),
            P(EP, None),
            P(EP, None, TP),
            P(EP, None, TP),
            P(EP, TP, None),
            P(None, TP),
            P(None, TP),
            P(TP, None),
            P(),
            P(None, ALL),
            P(None, ALL),
            P(ALL, None),
            P(),
        ),
        out_specs=(P(EP, None), P(EP, TP, None, None)),
        check_vma=False,
    )
```

```python
import jax
import jax.numpy as jnp
import numpy as np
from jax import lax
from jax.experimental import pallas as pl
from jax.experimental.pallas import tpu as pltpu
from jax.sharding import Mesh
from jax.sharding import PartitionSpec as P

HEADS = 8
EP = ("z", "x")
TP = ("y", "c")
ALL = ("z", "x", "y", "c")
NORM_EPS = 1e-05
RESIDUAL_SCALE = 2.0**0.5
BF = jnp.bfloat16
F32 = jnp.float32
VM = pl.BlockSpec(memory_space=pltpu.VMEM)
SM = pl.BlockSpec(memory_space=pltpu.SMEM)
HB = pl.BlockSpec(memory_space=pltpu.HBM)
NT = (((1,), (1,)), ((), ()))


def shifted(value, axis, step):
    n = lax.axis_size(axis)
    return lax.ppermute(value, axis, [(i, (i + step) % n) for i in range(n)])


def silu(v):
    return v / (1.0 + jnp.exp(-v))


def norm(inputs, gain):
    average = jnp.mean(inputs, axis=-1, keepdims=True)
    centered = inputs - average
    variance = jnp.mean(centered * centered, axis=-1, keepdims=True)
    return centered * lax.rsqrt(variance + NORM_EPS) * gain


def dot(a, b):
    return jnp.dot(a, b, preferred_element_type=F32)


def dot_nt(a, b):
    return lax.dot_general(a, b, NT, preferred_element_type=F32)


def columns_of(rows):
    n = rows.shape[0]
    return jnp.concatenate([rows, jnp.zeros((128 - n, 128), F32)], axis=0).T


def decay_row():
    head = (lax.axis_index("y") * 2 + lax.axis_index("c")).astype(F32)
    return 1.0 - jnp.exp2(-2.0 - 10.0 * jnp.full((1, 128), head, F32) / (HEADS - 1))


def mixer_kernel(
    lengths, frequency, tokens, gain, wq, wk, wv, wg, state, ow, ed, dd, sd,
    kept, given, key_out, value_out, d0, d1, d2, d3,
    bq, bk, bv, bg, bs, bo, rows, sems, dsems,
):
    moves = [
        pltpu.make_async_copy(src, dst, sems.at[i])
        for i, (src, dst) in enumerate(
            ((wq, bq), (wk, bk), (state, bs), (wv, bv), (wg, bg), (ow, bo))
        )
    ]
    for move in moves:
        move.start()
    slices = []
    for k, out in enumerate((d0, d1, d2, d3)):
        cols = pl.ds(pl.multiple_of(lax.rem(lax.axis_index("y") + k, 4) * 512, 512), 512)
        for src, dst in (
            (ed.at[0, :, cols], out.at[pl.ds(0, 64)]),
            (ed.at[1, :, cols], out.at[pl.ds(64, 64)]),
            (sd.at[:, cols], out.at[pl.ds(128, 64)]),
            (dd.at[:, cols], out.at[pl.ds(192, 32)]),
        ):
            c = pltpu.make_async_copy(src, dst, dsems.at[len(slices)])
            c.start()
            slices.append(c)
    f = frequency[...]
    for i in range(16):
        rows[i : i + 1, :] = jnp.full((1, 128), lengths[i].astype(F32), F32) * f
    angles = rows[...]
    lane = lax.broadcasted_iota(jnp.int32, (16, 128), 1)
    cos2 = jnp.cos(angles)
    sin2 = jnp.sin(angles) * jnp.where(lane < 64, -1.0, 1.0)
    decay = decay_row()
    t = tokens[...]

    def turned(v):
        return v * cos2 + pltpu.roll(v, 64, 1) * sin2

    moves[0].wait()
    q = turned(dot(t, bq[...]))
    qc = columns_of(q)
    moves[1].wait()
    k = turned(dot(t, bk[...]) * 128 ** (-0.5))
    key_out[...] = k
    moves[2].wait()
    for i in range(16):
        rows[i : i + 1, :] = jnp.sum(qc[:, i : i + 1] * bs[i], axis=0, keepdims=True)
    moves[3].wait()
    v = dot(t, bv[...])
    value_out[...] = v
    moves[4].wait()
    g = dot(t, bg[...])
    match = jnp.sum(q * k, axis=1, keepdims=True)
    readout = decay * rows[...] + match * v
    mixed = (norm(readout, gain[...]) * silu(g)).astype(BF)
    moves[5].wait()
    partial = dot(mixed, bo[...])
    low, high = partial[:8], partial[8:]
    first = lax.axis_index("c") == 0
    kept[...] = jnp.where(first, low, high).astype(BF)
    given[...] = jnp.where(first, high, low).astype(BF)
    for c in slices:
        c.wait()


def pack_kernel(*refs):
    own, peer, w_out, sems = refs[0:6], refs[6:12], refs[12], refs[13]
    moves = []

    def move(src, dst):
        c = pltpu.make_async_copy(src, dst, sems.at[len(moves)])
        c.start()
        moves.append(c)

    for side, (eg, eu, dg, du, sg, su) in enumerate((own, peer)):
        for half, (e, d, s) in enumerate(((eg, dg, sg), (eu, du, su))):
            o = 512 * side + 256 * half
            move(e.at[0], w_out.at[pl.ds(o, 64)])
            move(e.at[1], w_out.at[pl.ds(o + 64, 64)])
            move(d, w_out.at[pl.ds(o + 128, 32)])
            move(s, w_out.at[pl.ds(o + 160, 64)])
            move(d, w_out.at[pl.ds(o + 224, 32)])
    for c in moves:
        c.wait()


def arrange_kernel(y0, y1, y2, y3, p0, p1, p2, p3, out):
    for k, pair in enumerate(((y0, p0), (y1, p1), (y2, p2), (y3, p3))):
        for s, src in enumerate(pair):
            for j in range(3):
                o = 512 * j + 128 * k + 64 * s
                out[o : o + 64, :] = src[64 * j : 64 * j + 64, :]
            o = 1536 + 64 * k + 32 * s
            out[o : o + 32, :] = src[192:224, :]


def state_kernel(keys, values, state, new_state, bs, bn, sems):
    load = pltpu.make_async_copy(state, bs, sems.at[0])
    load.start()
    kc = columns_of(keys[...])
    decay = decay_row()
    load.wait()
    for i in range(16):
        bn[i] = decay * bs[i] + kc[:, i : i + 1] * values[i : i + 1, :]
    store = pltpu.make_async_copy(bn, new_state, sems.at[1])
    store.start()
    store.wait()


def after_kernel(pair, r1, r2, r3, tokens, gain, ids, ews, after, sent, table):
    first = lax.axis_index("c") == 0
    table[...] = jnp.zeros((128, 128), F32)
    w = ews[...]
    high = w.astype(BF).astype(F32)
    table[0:6, 0:16] = ids[...].astype(F32)
    table[8:14, 0:16] = high
    table[16:22, 0:16] = w - high
    f = table[...].T
    f = jnp.where(first, f[0:8], f[8:16]).astype(BF)
    t = tokens[...].astype(F32)
    mine = jnp.where(first, t[:8], t[8:])
    branch = pair[...].astype(F32)
    for r in (r1, r2, r3):
        branch = branch + r[...].astype(F32)
    a = norm(RESIDUAL_SCALE * mine + branch, gain[...]).astype(BF)
    after[...] = a
    for j in range(8):
        sent[j, :, 0:2048] = a
        sent[j, :, 2048:2176] = f


def hidden_kernel(b0, b1, b2, b3, w_all, side, h_out, pt_out, acts, info, xo, xp):
    for k, b in enumerate((b0, b1, b2, b3)):
        acts[64 * k : 64 * k + 64, :] = b[:, 0:2048]
        info[64 * k : 64 * k + 64, :] = b[:, 2048:2176].astype(F32)
    a = acts[...]
    lane = lax.broadcasted_iota(jnp.int32, (256, 128), 1)
    row = lax.broadcasted_iota(jnp.int32, (256, 128), 0)
    f = info[...]
    w = pltpu.roll(f, 128 - 8, 1) + pltpu.roll(f, 128 - 16, 1)
    zi = lax.axis_index("z")
    e0 = ((zi * 4 + lax.axis_index("x")) * 2).astype(F32)
    named = lane < 6
    m0 = jnp.logical_and(f == e0, named)
    m1 = jnp.logical_and(f == e0 + 1.0, named)
    s0 = jnp.sum(jnp.where(m0, w, 0.0), axis=1, keepdims=True)
    s1 = jnp.sum(jnp.where(m1, w, 0.0), axis=1, keepdims=True)
    a0 = jnp.sum(jnp.where(m0, 1.0, 0.0), axis=1, keepdims=True)
    a1 = jnp.sum(jnp.where(m1, 1.0, 0.0), axis=1, keepdims=True)
    flags = jnp.where(lane == 0, a0, jnp.where(lane == 1, a1, 0.0)).astype(BF)
    r2 = lax.broadcasted_iota(jnp.int32, (256, 256), 0)
    c2 = lax.broadcasted_iota(jnp.int32, (256, 256), 1)
    earlier = jnp.logical_and((r2 >> 3) == (c2 >> 3), c2 < r2)
    rank = dot(jnp.where(earlier, 1.0, 0.0).astype(BF), flags)
    base = ((row >> 3) * 2).astype(F32)
    lane_f = lane.astype(F32)
    t0 = jnp.logical_and(a0 > 0.5, base + rank[:, 0:1] == lane_f)
    t1 = jnp.logical_and(a1 > 0.5, base + rank[:, 1:2] == lane_f - 64.0)
    pt = jnp.where(jnp.where(lane < 64, jnp.where(t0, 1.0, 0.0), jnp.where(t1, 1.0, 0.0)) > 0.5, 1.0, 0.0)
    pt_out[...] = pt.astype(BF)
    pm = pt.T.astype(BF)

    switch = 1.0 / (1.0 + jnp.exp(-dot_nt(a, side[...])[:, 0:1]))
    share = jnp.where(lane < 64, s0, s1)

    def hidden_of(start, tail):
        gate = dot_nt(a, w_all[start : start + 256, :])
        up = dot_nt(a, w_all[start + 256 : start + 512, :])
        h = silu(gate) * up
        x = h[:, 128:256]
        tail[...] = x
        return (h[:, 0:128] * share).astype(BF), x * switch

    ho, do = hidden_of(0, xo)
    hp, dp = hidden_of(512, xp)
    eo = dot(pm, ho)
    ep = dot(pm, hp)
    lane1 = lane[:128]
    row1 = row[:128]
    near = lane1 < 64
    upper = jnp.where(near, eo, pltpu.roll(ep, 64, 1))
    lower = jnp.where(near, pltpu.roll(eo, 64, 1), ep)
    h_out[128:256, :] = jnp.where(row1 < 64, upper, lower).astype(BF)
    dense = jnp.where(lane < 32, do, pltpu.roll(dp, 32, 1))
    h_out[0:128, :] = jnp.where(near, dense[0:128], pltpu.roll(dense[128:256], 64, 1)).astype(BF)
    mine = pl.ds(pl.multiple_of(zi * 8, 8), 8)
    so, sp = xo[mine, :], xp[mine, :]
    s = jnp.where(lane[:8] < 64, pltpu.roll(so, 96, 1), pltpu.roll(sp, 32, 1))
    h_out[256:272, :] = jnp.concatenate([s, jnp.zeros((8, 128), F32)], axis=0).astype(BF)


def down_kernel(h0, h1, h2, h3, pt, d_all, out, shared):
    hs = (h0, h1, h2, h3)
    near = lax.broadcasted_iota(jnp.int32, (128, 128), 1) < 64
    total = None
    for n in range(2):
        u = hs[2 * n][0:128, :].astype(F32)
        v = hs[2 * n + 1][0:128, :].astype(F32)
        top = jnp.where(near, u, pltpu.roll(v, 64, 1))
        bottom = jnp.where(near, pltpu.roll(u, 64, 1), v)
        h = jnp.concatenate([top, bottom], axis=0).astype(BF)
        part = dot(h, d_all[1536 + 128 * n : 1664 + 128 * n, :])
        total = part if total is None else total + part
    outs = []
    for e in range(2):
        h = jnp.concatenate([r[128 + 64 * e : 192 + 64 * e, :] for r in hs], axis=1)
        outs.append(dot(h, d_all[512 * e : 512 * e + 512, :]))
    total = total + dot(pt[...], jnp.concatenate(outs, axis=0).astype(BF))
    h = jnp.concatenate([r[256:272, :] for r in hs], axis=1)
    shared[...] = dot(h, d_all[1024:1536, :])[0:8]
    for k in range(4):
        block = total[64 * k : 64 * k + 64].astype(BF).reshape(8, 8, 512)
        out[:, lax.rem(lax.axis_index("x") + 4 - k, 4)] = block


def sum_kernel(back, shared, out):
    total = shared[...]
    for j in range(32):
        total = total + back[j].astype(F32)
    for j in range(8):
        out[j] = total


def last_kernel(got, own, other, gain, out):
    first = lax.axis_index("c") == 0
    mine, theirs = own[...].astype(F32), other[...].astype(F32)
    low = jnp.where(first, mine, theirs)
    high = jnp.where(first, theirs, mine)
    rows = []
    for c, residual in enumerate((low, high)):
        side = jnp.concatenate([got[2 * y + c] for y in range(4)], axis=1)
        rows.append(norm(RESIDUAL_SCALE * residual + side, gain[...]))
    out[...] = jnp.concatenate(rows, axis=0).astype(BF)


def limit(mib):
    return pltpu.CompilerParams(vmem_limit_bytes=mib * 2**20)


def shape(*dims, dtype=BF):
    return pltpu.VMEM(dims, dtype)


def near(value):
    return pltpu.with_memory_space_constraint(value, pltpu.VMEM)


def big(value):
    return pltpu.with_memory_space_constraint(value, pltpu.HBM)


def layer(
    tokens,
    lengths,
    old_state,
    query_weight,
    key_weight,
    value_weight,
    gate_weight,
    head_gain,
    output_weight,
    first_gain,
    expert_ids,
    expert_weights,
    expert_gate,
    expert_up,
    expert_down,
    shared_gate,
    shared_up,
    shared_down,
    side_gate,
    dense_gate,
    dense_up,
    dense_down,
    second_gain,
):
    frequency = np.asarray(1.0 / 10000.0 ** ((np.arange(128) % 64) / 64.0), np.float32)
    state = old_state.reshape(16, 128, 128)
    kept, given, keys, values, *downs = pl.pallas_call(
        mixer_kernel,
        in_specs=[SM, VM, VM, VM] + [HB] * 9,
        out_specs=[VM] * 8,
        out_shape=[shape(8, 2048)] * 2 + [shape(16, 128, dtype=F32)] * 2 + [shape(224, 512)] * 4,
        scratch_shapes=[pltpu.VMEM((2048, 128), BF)] * 4
        + [
            pltpu.VMEM((16, 128, 128), F32),
            pltpu.VMEM((128, 2048), BF),
            pltpu.VMEM((16, 128), F32),
            pltpu.SemaphoreType.DMA((6,)),
            pltpu.SemaphoreType.DMA((16,)),
        ],
        compiler_params=limit(8),
        name="mixer",
    )(
        big(lengths), big(jnp.asarray(frequency)[None]), big(tokens), big(head_gain.reshape(1, 128)),
        big(query_weight), big(key_weight), big(value_weight), big(gate_weight), big(state),
        big(output_weight), big(expert_down), big(dense_down), big(shared_down),
    )

    pair = (kept.astype(F32) + shifted(given, "c", 1).astype(F32)).astype(BF)
    raw = (
        expert_gate.transpose(0, 2, 1), expert_up.transpose(0, 2, 1),
        dense_gate.T, dense_up.T, shared_gate.T, shared_up.T,
    )
    side = jnp.broadcast_to(side_gate[None], (8, 2048))
    raw, side, pair = lax.optimization_barrier((raw, side, pair))
    arrived = [shifted(pair, "y", k) for k in range(1, 4)]
    peers = [shifted(r, "c", 1) for r in raw]
    after, sent = pl.pallas_call(
        after_kernel,
        in_specs=[VM] * 8,
        out_specs=[VM, VM],
        out_shape=[shape(8, 2048), jax.ShapeDtypeStruct((8, 8, 2176), BF)],
        scratch_shapes=[pltpu.VMEM((128, 128), F32)],
        compiler_params=limit(4),
        name="after",
    )(
        pair, *arrived, big(tokens), big(first_gain.reshape(1, 2048)),
        big(expert_ids.T), big(expert_weights.T),
    )

    peers, downs, side, sent = lax.optimization_barrier((peers, downs, side, sent))
    block = lax.all_to_all(sent, "z", 0, 0, tiled=True).reshape(64, 2176)
    from_y = [downs[0]] + [shifted(downs[k], "y", k) for k in range(1, 4)]
    blocks = [block] + [shifted(block, "x", k) for k in range(1, 4)]
    other = shifted(after, "c", 1)
    from_c = [shifted(d, "c", 1) for d in from_y]
    w_all = pl.pallas_call(
        pack_kernel,
        in_specs=[HB] * 12,
        out_specs=VM,
        out_shape=shape(1024, 2048),
        scratch_shapes=[pltpu.SemaphoreType.DMA((20,))],
        compiler_params=limit(2),
        name="pack",
    )(*[big(v) for v in raw], *peers)
    new_state = pl.pallas_call(
        state_kernel,
        in_specs=[VM, VM, HB],
        out_specs=HB,
        out_shape=pltpu.HBM((16, 128, 128), F32),
        scratch_shapes=[
            pltpu.VMEM((16, 128, 128), F32),
            pltpu.VMEM((16, 128, 128), F32),
            pltpu.SemaphoreType.DMA((2,)),
        ],
        compiler_params=limit(4),
        name="state",
    )(keys, values, big(state))

    hidden, slots = pl.pallas_call(
        hidden_kernel,
        in_specs=[VM] * 6,
        out_specs=[VM] * 2,
        out_shape=[shape(272, 128), shape(256, 128)],
        scratch_shapes=[
            pltpu.VMEM((256, 2048), BF),
            pltpu.VMEM((256, 128), F32),
            pltpu.VMEM((256, 128), F32),
            pltpu.VMEM((256, 128), F32),
        ],
        compiler_params=limit(8),
        name="hidden",
    )(*blocks, near(w_all), side)
    gathered = [hidden] + [shifted(hidden, "y", k) for k in range(1, 4)]
    d_all = pl.pallas_call(
        arrange_kernel,
        in_specs=[VM] * 8,
        out_specs=VM,
        out_shape=shape(1792, 512),
        compiler_params=limit(2),
        name="arrange",
    )(*from_y, *from_c)
    partial, shared = pl.pallas_call(
        down_kernel,
        in_specs=[VM] * 6,
        out_specs=[VM, VM],
        out_shape=[shape(8, 4, 8, 512), shape(8, 512, dtype=F32)],
        compiler_params=limit(6),
        name="down",
    )(*gathered, slots, near(d_all))

    back = lax.all_to_all(partial.reshape(32, 8, 512), EP, 0, 0, tiled=True)
    mine = pl.pallas_call(
        sum_kernel,
        in_specs=[VM, VM],
        out_specs=VM,
        out_shape=jax.ShapeDtypeStruct((8, 8, 512), F32),
        compiler_params=limit(3),
        name="sum",
    )(back, shared)
    got = lax.all_to_all(mine, TP, 0, 0, tiled=True)
    layer_out = pl.pallas_call(
        last_kernel,
        in_specs=[VM] * 4,
        out_specs=VM,
        out_shape=jax.ShapeDtypeStruct((16, 2048), BF),
        compiler_params=limit(3),
        name="last",
    )(got, after, other, big(second_gain.reshape(1, 2048)))
    return (layer_out, new_state.reshape(16, 1, 128, 128))


def solution(mesh):
    finer = Mesh(mesh.devices.reshape(8, 4, 4, 2), ALL)
    return jax.shard_map(
        layer,
        mesh=finer,
        in_specs=(
            P(EP, None),
            P(EP),
            P(EP, TP, None, None),
            P(None, TP),
            P(None, TP),
            P(None, TP),
            P(None, TP),
            P(TP),
            P(TP, None),
            P(),
            P(EP, None),
            P(EP, None),
            P(EP, None, TP),
            P(EP, None, TP),
            P(EP, TP, None),
            P(None, TP),
            P(None, TP),
            P(TP, None),
            P(),
            P(None, ALL),
            P(None, ALL),
            P(ALL, None),
            P(),
        ),
        out_specs=(P(EP, None), P(EP, TP, None, None)),
        check_vma=False,
    )
```

```python
import jax
import jax.numpy as jnp
import numpy as np
from jax import lax
from jax.experimental import pallas as pl
from jax.experimental.pallas import tpu as pltpu
from jax.sharding import Mesh
from jax.sharding import PartitionSpec as P

HEADS = 8
EP = ("z", "x")
TP = ("y", "c")
ALL = ("z", "x", "y", "c")
NORM_EPS = 1e-05
RESIDUAL_SCALE = 2.0**0.5
BF = jnp.bfloat16
F32 = jnp.float32
VM = pl.BlockSpec(memory_space=pltpu.VMEM)
SM = pl.BlockSpec(memory_space=pltpu.SMEM)
HB = pl.BlockSpec(memory_space=pltpu.HBM)
NT = (((1,), (1,)), ((), ()))


def shifted(value, axis, step):
    n = lax.axis_size(axis)
    return lax.ppermute(value, axis, [(i, (i + step) % n) for i in range(n)])


def silu(v):
    return v / (1.0 + jnp.exp(-v))


def norm(inputs, gain):
    average = jnp.mean(inputs, axis=-1, keepdims=True)
    centered = inputs - average
    variance = jnp.mean(centered * centered, axis=-1, keepdims=True)
    return centered * lax.rsqrt(variance + NORM_EPS) * gain


def dot(a, b):
    return jnp.dot(a, b, preferred_element_type=F32)


def dot_nt(a, b):
    return lax.dot_general(a, b, NT, preferred_element_type=F32)


def columns_of(rows):
    n = rows.shape[0]
    return jnp.concatenate([rows, jnp.zeros((128 - n, 128), F32)], axis=0).T


def decay_row():
    head = (lax.axis_index("y") * 2 + lax.axis_index("c")).astype(F32)
    return 1.0 - jnp.exp2(-2.0 - 10.0 * jnp.full((1, 128), head, F32) / (HEADS - 1))


def mixer_kernel(
    lengths, frequency, tokens, gain, wq, wk, wv, wg, state, ow, ed, dd, sd, ids, ews, gain1, gain2,
    kept, given, key_out, value_out, d0, d1, d2, d3, mine, info, g1, g2,
    bl, bf, bt, bn, bq, bk, bv, bg, bs, bo, bi, bw, rows, table, sems, dsems,
):
    moves = [
        pltpu.make_async_copy(src, dst, sems.at[i])
        for i, (src, dst) in enumerate(
            (
                (wq, bq), (wk, bk), (state, bs), (wv, bv), (wg, bg), (ow, bo),
                (lengths, bl), (frequency, bf), (tokens, bt), (gain, bn),
                (ids, bi), (ews, bw), (gain1, g1), (gain2, g2),
            )
        )
    ]
    for i in (6, 7, 8, 0, 1, 2, 3, 4, 5, 9, 10, 11, 12, 13):
        moves[i].start()
    slices = []
    for k, out in enumerate((d0, d1, d2, d3)):
        cols = pl.ds(pl.multiple_of(lax.rem(lax.axis_index("y") + k, 4) * 512, 512), 512)
        for src, dst in (
            (ed.at[0, :, cols], out.at[pl.ds(0, 64)]),
            (ed.at[1, :, cols], out.at[pl.ds(64, 64)]),
            (sd.at[:, cols], out.at[pl.ds(128, 64)]),
            (dd.at[:, cols], out.at[pl.ds(192, 32)]),
        ):
            c = pltpu.make_async_copy(src, dst, dsems.at[len(slices)])
            c.start()
            slices.append(c)
    first = lax.axis_index("c") == 0
    moves[6].wait()
    moves[7].wait()
    f = bf[...]
    for i in range(16):
        rows[i : i + 1, :] = jnp.full((1, 128), bl[i].astype(F32), F32) * f
    angles = rows[...]
    lane = lax.broadcasted_iota(jnp.int32, (16, 128), 1)
    cos2 = jnp.cos(angles)
    sin2 = jnp.sin(angles) * jnp.where(lane < 64, -1.0, 1.0)
    decay = decay_row()
    moves[8].wait()
    t = bt[...]
    wide = t.astype(F32)
    mine[...] = jnp.where(first, wide[:8], wide[8:]).astype(BF)

    def turned(v):
        return v * cos2 + pltpu.roll(v, 64, 1) * sin2

    moves[0].wait()
    q = turned(dot(t, bq[...]))
    qc = columns_of(q)
    moves[1].wait()
    k = turned(dot(t, bk[...]) * 128 ** (-0.5))
    key_out[...] = k
    moves[2].wait()
    for i in range(16):
        rows[i : i + 1, :] = jnp.sum(qc[:, i : i + 1] * bs[i], axis=0, keepdims=True)
    moves[3].wait()
    v = dot(t, bv[...])
    value_out[...] = v
    moves[4].wait()
    g = dot(t, bg[...])
    match = jnp.sum(q * k, axis=1, keepdims=True)
    readout = decay * rows[...] + match * v
    moves[9].wait()
    mixed = (norm(readout, bn[...]) * silu(g)).astype(BF)
    moves[5].wait()
    partial = dot(mixed, bo[...])
    low, high = partial[:8], partial[8:]
    kept[...] = jnp.where(first, low, high).astype(BF)
    given[...] = jnp.where(first, high, low).astype(BF)
    moves[10].wait()
    moves[11].wait()
    table[...] = jnp.zeros((128, 128), F32)
    w = bw[...]
    top = w.astype(BF).astype(F32)
    table[0:6, 0:16] = bi[...].astype(F32)
    table[8:14, 0:16] = top
    table[16:22, 0:16] = w - top
    f = table[...].T
    info[...] = jnp.where(first, f[0:8], f[8:16]).astype(BF)
    for c in (moves[12], moves[13], *slices):
        c.wait()


def pack_kernel(*refs):
    own, peer, w_out, sems = refs[0:6], refs[6:12], refs[12], refs[13]
    moves = []

    def move(src, dst):
        c = pltpu.make_async_copy(src, dst, sems.at[len(moves)])
        c.start()
        moves.append(c)

    for side, (eg, eu, dg, du, sg, su) in enumerate((own, peer)):
        for half, (e, d, s) in enumerate(((eg, dg, sg), (eu, du, su))):
            o = 512 * side + 256 * half
            move(e.at[0], w_out.at[pl.ds(o, 64)])
            move(e.at[1], w_out.at[pl.ds(o + 64, 64)])
            move(d, w_out.at[pl.ds(o + 128, 32)])
            move(s, w_out.at[pl.ds(o + 160, 64)])
            move(d, w_out.at[pl.ds(o + 224, 32)])
    for c in moves:
        c.wait()


def arrange_kernel(y0, y1, y2, y3, p0, p1, p2, p3, out):
    for k, pair in enumerate(((y0, p0), (y1, p1), (y2, p2), (y3, p3))):
        for s, src in enumerate(pair):
            for j in range(3):
                o = 512 * j + 128 * k + 64 * s
                out[o : o + 64, :] = src[64 * j : 64 * j + 64, :]
            o = 1536 + 64 * k + 32 * s
            out[o : o + 32, :] = src[192:224, :]


def state_kernel(keys, values, state, new_state, bs, bn, sems):
    load = pltpu.make_async_copy(state, bs, sems.at[0])
    load.start()
    kc = columns_of(keys[...])
    decay = decay_row()
    load.wait()
    for i in range(16):
        bn[i] = decay * bs[i] + kc[:, i : i + 1] * values[i : i + 1, :]
    store = pltpu.make_async_copy(bn, new_state, sems.at[1])
    store.start()
    store.wait()


def after_kernel(pair, r1, r2, r3, mine, gain, info, after, sent):
    branch = pair[...].astype(F32)
    for r in (r1, r2, r3):
        branch = branch + r[...].astype(F32)
    a = norm(RESIDUAL_SCALE * mine[...].astype(F32) + branch, gain[...]).astype(BF)
    after[...] = a
    f = info[...]
    for j in range(8):
        sent[j, :, 0:2048] = a
        sent[j, :, 2048:2176] = f


def hidden_kernel(b0, b1, b3, near_half, far_half, w_all, side, h_out, pt_out, acts, info, xo, xp):
    for k, b in ((0, b0), (1, b1), (3, b3)):
        acts[64 * k : 64 * k + 64, :] = b[:, 0:2048]
        info[64 * k : 64 * k + 64, :] = b[:, 2048:2176].astype(F32)
    odd = lax.rem(lax.axis_index("y"), 2) * 32
    for start, b in ((128 + odd, near_half), (160 - odd, far_half)):
        here = pl.ds(pl.multiple_of(start, 32), 32)
        acts[here, :] = b[:, 0:2048]
        info[here, :] = b[:, 2048:2176].astype(F32)
    a = acts[...]
    lane = lax.broadcasted_iota(jnp.int32, (256, 128), 1)
    row = lax.broadcasted_iota(jnp.int32, (256, 128), 0)
    f = info[...]
    w = pltpu.roll(f, 128 - 8, 1) + pltpu.roll(f, 128 - 16, 1)
    zi = lax.axis_index("z")
    e0 = ((zi * 4 + lax.axis_index("x")) * 2).astype(F32)
    named = lane < 6
    m0 = jnp.logical_and(f == e0, named)
    m1 = jnp.logical_and(f == e0 + 1.0, named)
    s0 = jnp.sum(jnp.where(m0, w, 0.0), axis=1, keepdims=True)
    s1 = jnp.sum(jnp.where(m1, w, 0.0), axis=1, keepdims=True)
    a0 = jnp.sum(jnp.where(m0, 1.0, 0.0), axis=1, keepdims=True)
    a1 = jnp.sum(jnp.where(m1, 1.0, 0.0), axis=1, keepdims=True)
    flags = jnp.where(lane == 0, a0, jnp.where(lane == 1, a1, 0.0)).astype(BF)
    r2 = lax.broadcasted_iota(jnp.int32, (256, 256), 0)
    c2 = lax.broadcasted_iota(jnp.int32, (256, 256), 1)
    earlier = jnp.logical_and((r2 >> 3) == (c2 >> 3), c2 < r2)
    rank = dot(jnp.where(earlier, 1.0, 0.0).astype(BF), flags)
    base = ((row >> 3) * 2).astype(F32)
    lane_f = lane.astype(F32)
    t0 = jnp.logical_and(a0 > 0.5, base + rank[:, 0:1] == lane_f)
    t1 = jnp.logical_and(a1 > 0.5, base + rank[:, 1:2] == lane_f - 64.0)
    pt = jnp.where(jnp.where(lane < 64, jnp.where(t0, 1.0, 0.0), jnp.where(t1, 1.0, 0.0)) > 0.5, 1.0, 0.0)
    pt_out[...] = pt.astype(BF)
    pm = pt.T.astype(BF)

    switch = 1.0 / (1.0 + jnp.exp(-dot_nt(a, side[...])[:, 0:1]))
    share = jnp.where(lane < 64, s0, s1)

    def hidden_of(start, tail):
        gate = dot_nt(a, w_all[start : start + 256, :])
        up = dot_nt(a, w_all[start + 256 : start + 512, :])
        h = silu(gate) * up
        x = h[:, 128:256]
        tail[...] = x
        return (h[:, 0:128] * share).astype(BF), x * switch

    ho, do = hidden_of(0, xo)
    hp, dp = hidden_of(512, xp)
    eo = dot(pm, ho)
    ep = dot(pm, hp)
    lane1 = lane[:128]
    row1 = row[:128]
    near = lane1 < 64
    upper = jnp.where(near, eo, pltpu.roll(ep, 64, 1))
    lower = jnp.where(near, pltpu.roll(eo, 64, 1), ep)
    h_out[128:256, :] = jnp.where(row1 < 64, upper, lower).astype(BF)
    dense = jnp.where(lane < 32, do, pltpu.roll(dp, 32, 1))
    h_out[0:128, :] = jnp.where(near, dense[0:128], pltpu.roll(dense[128:256], 64, 1)).astype(BF)
    mine = pl.ds(pl.multiple_of(zi * 8, 8), 8)
    so, sp = xo[mine, :], xp[mine, :]
    s = jnp.where(lane[:8] < 64, pltpu.roll(so, 96, 1), pltpu.roll(sp, 32, 1))
    h_out[256:272, :] = jnp.concatenate([s, jnp.zeros((8, 128), F32)], axis=0).astype(BF)


def down_kernel(h0, h1, h2, h3, pt, d_all, out, shared):
    hs = (h0, h1, h2, h3)
    near = lax.broadcasted_iota(jnp.int32, (128, 128), 1) < 64
    total = None
    for n in range(2):
        u = hs[2 * n][0:128, :].astype(F32)
        v = hs[2 * n + 1][0:128, :].astype(F32)
        top = jnp.where(near, u, pltpu.roll(v, 64, 1))
        bottom = jnp.where(near, pltpu.roll(u, 64, 1), v)
        h = jnp.concatenate([top, bottom], axis=0).astype(BF)
        part = dot(h, d_all[1536 + 128 * n : 1664 + 128 * n, :])
        total = part if total is None else total + part
    outs = []
    for e in range(2):
        h = jnp.concatenate([r[128 + 64 * e : 192 + 64 * e, :] for r in hs], axis=1)
        outs.append(dot(h, d_all[512 * e : 512 * e + 512, :]))
    total = total + dot(pt[...], jnp.concatenate(outs, axis=0).astype(BF))
    h = jnp.concatenate([r[256:272, :] for r in hs], axis=1)
    shared[...] = dot(h, d_all[1024:1536, :])[0:8]
    for k in range(4):
        block = total[64 * k : 64 * k + 64].astype(BF).reshape(8, 8, 512)
        out[:, lax.rem(lax.axis_index("x") + 4 - k, 4)] = block


def sum_kernel(back, shared, out):
    total = shared[...]
    for j in range(32):
        total = total + back[j].astype(F32)
    out[...] = total


def last_kernel(s0, s1, s2, s3, after, gain, out, whole):
    for k, s in enumerate((s0, s1, s2, s3)):
        start = lax.rem(lax.axis_index("y") + 4 - k, 4) * 512
        whole[:, pl.ds(pl.multiple_of(start, 512), 512)] = s[...]
    out[...] = norm(RESIDUAL_SCALE * after[...].astype(F32) + whole[...], gain[...]).astype(BF)


def join_kernel(own, other, out):
    first = lax.axis_index("c") == 0
    a, b = own[...].astype(F32), other[...].astype(F32)
    low = jnp.where(first, a, b)
    high = jnp.where(first, b, a)
    out[...] = jnp.concatenate([low, high], axis=0).astype(BF)


def limit(mib):
    return pltpu.CompilerParams(vmem_limit_bytes=mib * 2**20)


def shape(*dims, dtype=BF):
    return pltpu.VMEM(dims, dtype)


def near(value):
    return pltpu.with_memory_space_constraint(value, pltpu.VMEM)


def big(value):
    return pltpu.with_memory_space_constraint(value, pltpu.HBM)


def layer(
    tokens,
    lengths,
    old_state,
    query_weight,
    key_weight,
    value_weight,
    gate_weight,
    head_gain,
    output_weight,
    first_gain,
    expert_ids,
    expert_weights,
    expert_gate,
    expert_up,
    expert_down,
    shared_gate,
    shared_up,
    shared_down,
    side_gate,
    dense_gate,
    dense_up,
    dense_down,
    second_gain,
):
    frequency = np.asarray(1.0 / 10000.0 ** ((np.arange(128) % 64) / 64.0), np.float32)
    state = old_state.reshape(16, 128, 128)
    outs = pl.pallas_call(
        mixer_kernel,
        in_specs=[HB] * 17,
        out_specs=[VM] * 12,
        out_shape=[shape(8, 2048)] * 2
        + [shape(16, 128, dtype=F32)] * 2
        + [shape(224, 512)] * 4
        + [shape(8, 2048), shape(8, 128)]
        + [shape(1, 2048, dtype=F32)] * 2,
        scratch_shapes=[
            pltpu.SMEM((16,), jnp.int32),
            pltpu.VMEM((1, 128), F32),
            pltpu.VMEM((16, 2048), BF),
            pltpu.VMEM((1, 128), F32),
        ]
        + [pltpu.VMEM((2048, 128), BF)] * 4
        + [
            pltpu.VMEM((16, 128, 128), F32),
            pltpu.VMEM((128, 2048), BF),
            pltpu.VMEM((6, 16), jnp.int32),
            pltpu.VMEM((6, 16), F32),
            pltpu.VMEM((16, 128), F32),
            pltpu.VMEM((128, 128), F32),
            pltpu.SemaphoreType.DMA((14,)),
            pltpu.SemaphoreType.DMA((16,)),
        ],
        compiler_params=limit(8),
        name="mixer",
    )(
        *[
            big(v)
            for v in (
                lengths, jnp.asarray(frequency)[None], tokens, head_gain.reshape(1, 128),
                query_weight, key_weight, value_weight, gate_weight, state, output_weight,
                expert_down, dense_down, shared_down, expert_ids.T, expert_weights.T,
                first_gain.reshape(1, 2048), second_gain.reshape(1, 2048),
            )
        ]
    )
    kept, given, keys, values = outs[0:4]
    downs, (mine, info, g1, g2) = outs[4:8], outs[8:12]

    pair = (kept.astype(F32) + shifted(given, "c", 1).astype(F32)).astype(BF)
    raw = (
        expert_gate.transpose(0, 2, 1), expert_up.transpose(0, 2, 1),
        dense_gate.T, dense_up.T, shared_gate.T, shared_up.T,
    )
    side = jnp.broadcast_to(side_gate[None], (8, 2048))
    side, downs, pair = lax.optimization_barrier((side, downs, pair))
    arrived = [shifted(pair, "y", k) for k in range(1, 4)]
    from_y = [downs[0]] + [shifted(downs[k], "y", k) for k in range(1, 4)]
    after, sent = pl.pallas_call(
        after_kernel,
        in_specs=[VM] * 7,
        out_specs=[VM, VM],
        out_shape=[shape(8, 2048), jax.ShapeDtypeStruct((8, 8, 2176), BF)],
        compiler_params=limit(4),
        name="after",
    )(pair, *arrived, mine, g1, info)

    raw, side, sent = lax.optimization_barrier((raw, side, sent))
    peers = [shifted(r, "c", 1) for r in raw]
    block = lax.all_to_all(sent, "z", 0, 0, tiled=True).reshape(64, 2176)
    part = lax.dynamic_slice_in_dim(block, (lax.axis_index("y") % 2) * 32, 32, 0)
    near_half = shifted(part, "x", 2)
    far_half = lax.ppermute(near_half, "y", [(0, 1), (1, 0), (2, 3), (3, 2)])
    blocks = [block] + [shifted(block, "x", k) for k in (1, 3)] + [near_half, far_half]
    from_c = [shifted(d, "c", 1) for d in from_y]
    w_all = pl.pallas_call(
        pack_kernel,
        in_specs=[HB] * 12,
        out_specs=VM,
        out_shape=shape(1024, 2048),
        scratch_shapes=[pltpu.SemaphoreType.DMA((20,))],
        compiler_params=limit(2),
        name="pack",
    )(*[big(v) for v in raw], *peers)
    new_state = pl.pallas_call(
        state_kernel,
        in_specs=[VM, VM, HB],
        out_specs=HB,
        out_shape=pltpu.HBM((16, 128, 128), F32),
        scratch_shapes=[
            pltpu.VMEM((16, 128, 128), F32),
            pltpu.VMEM((16, 128, 128), F32),
            pltpu.SemaphoreType.DMA((2,)),
        ],
        compiler_params=limit(4),
        name="state",
    )(keys, values, big(state))

    hidden, slots = pl.pallas_call(
        hidden_kernel,
        in_specs=[VM] * 7,
        out_specs=[VM] * 2,
        out_shape=[shape(272, 128), shape(256, 128)],
        scratch_shapes=[
            pltpu.VMEM((256, 2048), BF),
            pltpu.VMEM((256, 128), F32),
            pltpu.VMEM((256, 128), F32),
            pltpu.VMEM((256, 128), F32),
        ],
        compiler_params=limit(8),
        name="hidden",
    )(*blocks, near(w_all), side)
    gathered = [hidden] + [shifted(hidden, "y", k) for k in range(1, 4)]
    d_all = pl.pallas_call(
        arrange_kernel,
        in_specs=[VM] * 8,
        out_specs=VM,
        out_shape=shape(1792, 512),
        compiler_params=limit(2),
        name="arrange",
    )(*from_y, *from_c)
    partial, shared = pl.pallas_call(
        down_kernel,
        in_specs=[VM] * 6,
        out_specs=[VM, VM],
        out_shape=[shape(8, 4, 8, 512), shape(8, 512, dtype=F32)],
        compiler_params=limit(6),
        name="down",
    )(*gathered, slots, near(d_all))

    back = lax.all_to_all(partial.reshape(32, 8, 512), EP, 0, 0, tiled=True)
    total = pl.pallas_call(
        sum_kernel,
        in_specs=[VM, VM],
        out_specs=VM,
        out_shape=shape(8, 512, dtype=F32),
        compiler_params=limit(3),
        name="sum",
    )(back, shared)
    pieces = [total] + [shifted(total, "y", k) for k in range(1, 4)]
    final = pl.pallas_call(
        last_kernel,
        in_specs=[VM] * 6,
        out_specs=VM,
        out_shape=shape(8, 2048),
        scratch_shapes=[pltpu.VMEM((8, 2048), F32)],
        compiler_params=limit(3),
        name="last",
    )(*pieces, after, g2)
    layer_out = pl.pallas_call(
        join_kernel,
        in_specs=[VM] * 2,
        out_specs=VM,
        out_shape=jax.ShapeDtypeStruct((16, 2048), BF),
        compiler_params=limit(3),
        name="join",
    )(final, shifted(final, "c", 1))
    return (layer_out, new_state.reshape(16, 1, 128, 128))


def solution(mesh):
    finer = Mesh(mesh.devices.reshape(8, 4, 4, 2), ALL)
    return jax.shard_map(
        layer,
        mesh=finer,
        in_specs=(
            P(EP, None),
            P(EP),
            P(EP, TP, None, None),
            P(None, TP),
            P(None, TP),
            P(None, TP),
            P(None, TP),
            P(TP),
            P(TP, None),
            P(),
            P(EP, None),
            P(EP, None),
            P(EP, None, TP),
            P(EP, None, TP),
            P(EP, TP, None),
            P(None, TP),
            P(None, TP),
            P(TP, None),
            P(),
            P(None, ALL),
            P(None, ALL),
            P(ALL, None),
            P(),
        ),
        out_specs=(P(EP, None), P(EP, TP, None, None)),
        check_vma=False,
    )
```

```python
import jax
import jax.numpy as jnp
import numpy as np
from jax import lax
from jax.experimental import pallas as pl
from jax.experimental.pallas import tpu as pltpu
from jax.sharding import Mesh
from jax.sharding import PartitionSpec as P

HEADS = 8
EP = ("z", "x")
TP = ("y", "c")
ALL = ("z", "x", "y", "c")
NORM_EPS = 1e-05
RESIDUAL_SCALE = 2.0**0.5
BF = jnp.bfloat16
F32 = jnp.float32
VM = pl.BlockSpec(memory_space=pltpu.VMEM)
SM = pl.BlockSpec(memory_space=pltpu.SMEM)
HB = pl.BlockSpec(memory_space=pltpu.HBM)
NT = (((1,), (1,)), ((), ()))


def shifted(value, axis, step):
    n = lax.axis_size(axis)
    return lax.ppermute(value, axis, [(i, (i + step) % n) for i in range(n)])


def silu(v):
    return v / (1.0 + jnp.exp(-v))


def norm(inputs, gain):
    average = jnp.mean(inputs, axis=-1, keepdims=True)
    centered = inputs - average
    variance = jnp.mean(centered * centered, axis=-1, keepdims=True)
    return centered * lax.rsqrt(variance + NORM_EPS) * gain


def dot(a, b):
    return jnp.dot(a, b, preferred_element_type=F32)


def dot_nt(a, b):
    return lax.dot_general(a, b, NT, preferred_element_type=F32)


def columns_of(rows):
    n = rows.shape[0]
    return jnp.concatenate([rows, jnp.zeros((128 - n, 128), F32)], axis=0).T


def decay_row():
    head = (lax.axis_index("y") * 2 + lax.axis_index("c")).astype(F32)
    return 1.0 - jnp.exp2(-2.0 - 10.0 * jnp.full((1, 128), head, F32) / (HEADS - 1))


def mixer_kernel(
    lengths, frequency, tokens, gain, wq, wk, wv, wg, state, ow, ed, dd, sd, ids, ews, gain1,
    kept, given, key_out, value_out, d0, d1, d2, d3, mine, info, g1,
    bl, bf, bt, bn, bq, bk, bv, bg, bs, bo, bi, bw, rows, table, sems, dsems,
):
    moves = [
        pltpu.make_async_copy(src, dst, sems.at[i])
        for i, (src, dst) in enumerate(
            (
                (wq, bq), (wk, bk), (state, bs), (wv, bv), (wg, bg), (ow, bo),
                (lengths, bl), (frequency, bf), (tokens, bt), (gain, bn),
                (ids, bi), (ews, bw), (gain1, g1),
            )
        )
    ]
    for i in (6, 7, 8, 0, 1, 2, 3, 4, 5, 9, 10, 11, 12):
        moves[i].start()
    slices = []
    for k, out in enumerate((d0, d1, d2, d3)):
        cols = pl.ds(pl.multiple_of(lax.rem(lax.axis_index("y") + k, 4) * 512, 512), 512)
        for src, dst in (
            (ed.at[0, :, cols], out.at[pl.ds(0, 64)]),
            (ed.at[1, :, cols], out.at[pl.ds(64, 64)]),
            (sd.at[:, cols], out.at[pl.ds(128, 64)]),
            (dd.at[:, cols], out.at[pl.ds(192, 32)]),
        ):
            c = pltpu.make_async_copy(src, dst, dsems.at[len(slices)])
            c.start()
            slices.append(c)
    first = lax.axis_index("c") == 0
    moves[6].wait()
    moves[7].wait()
    f = bf[...]
    for i in range(16):
        rows[i : i + 1, :] = jnp.full((1, 128), bl[i].astype(F32), F32) * f
    angles = rows[...]
    lane = lax.broadcasted_iota(jnp.int32, (16, 128), 1)
    cos2 = jnp.cos(angles)
    sin2 = jnp.sin(angles) * jnp.where(lane < 64, -1.0, 1.0)
    decay = decay_row()
    moves[8].wait()
    t = bt[...]
    wide = t.astype(F32)
    mine[...] = jnp.where(first, wide[:8], wide[8:]).astype(BF)

    def turned(v):
        return v * cos2 + pltpu.roll(v, 64, 1) * sin2

    moves[0].wait()
    q = turned(dot(t, bq[...]))
    qc = columns_of(q)
    moves[1].wait()
    k = turned(dot(t, bk[...]) * 128 ** (-0.5))
    key_out[...] = k
    moves[2].wait()
    for i in range(16):
        rows[i : i + 1, :] = jnp.sum(qc[:, i : i + 1] * bs[i], axis=0, keepdims=True)
    moves[3].wait()
    v = dot(t, bv[...])
    value_out[...] = v
    moves[4].wait()
    g = dot(t, bg[...])
    match = jnp.sum(q * k, axis=1, keepdims=True)
    readout = decay * rows[...] + match * v
    moves[9].wait()
    mixed = (norm(readout, bn[...]) * silu(g)).astype(BF)
    moves[5].wait()
    partial = dot(mixed, bo[...])
    low, high = partial[:8], partial[8:]
    kept[...] = jnp.where(first, low, high).astype(BF)
    given[...] = jnp.where(first, high, low).astype(BF)
    moves[10].wait()
    moves[11].wait()
    table[...] = jnp.zeros((128, 128), F32)
    w = bw[...]
    top = w.astype(BF).astype(F32)
    table[0:6, 0:16] = bi[...].astype(F32)
    table[8:14, 0:16] = top
    table[16:22, 0:16] = w - top
    f = table[...].T
    info[...] = jnp.where(first, f[0:8], f[8:16]).astype(BF)
    for c in (moves[12], *slices):
        c.wait()


def pack_kernel(*refs):
    own, peer, w_out, sems = refs[0:6], refs[6:12], refs[12], refs[13]
    moves = []

    def move(src, dst):
        c = pltpu.make_async_copy(src, dst, sems.at[len(moves)])
        c.start()
        moves.append(c)

    for side, (eg, eu, dg, du, sg, su) in enumerate((own, peer)):
        for half, (e, d, s) in enumerate(((eg, dg, sg), (eu, du, su))):
            o = 512 * side + 256 * half
            move(e.at[0], w_out.at[pl.ds(o, 64)])
            move(e.at[1], w_out.at[pl.ds(o + 64, 64)])
            move(d, w_out.at[pl.ds(o + 128, 32)])
            move(s, w_out.at[pl.ds(o + 160, 64)])
            move(d, w_out.at[pl.ds(o + 224, 32)])
    for c in moves:
        c.wait()


def arrange_kernel(y0, y1, y2, y3, p0, p1, p2, p3, gain, out, gain_out, sem):
    move = pltpu.make_async_copy(gain, gain_out, sem.at[0])
    move.start()
    for k, pair in enumerate(((y0, p0), (y1, p1), (y2, p2), (y3, p3))):
        for s, src in enumerate(pair):
            for j in range(3):
                o = 512 * j + 128 * k + 64 * s
                out[o : o + 64, :] = src[64 * j : 64 * j + 64, :]
            o = 1536 + 64 * k + 32 * s
            out[o : o + 32, :] = src[192:224, :]
    move.wait()


def state_kernel(keys, values, state, new_state, bs, bn, sems):
    load = pltpu.make_async_copy(state, bs, sems.at[0])
    load.start()
    kc = columns_of(keys[...])
    decay = decay_row()
    load.wait()
    for i in range(16):
        bn[i] = decay * bs[i] + kc[:, i : i + 1] * values[i : i + 1, :]
    store = pltpu.make_async_copy(bn, new_state, sems.at[1])
    store.start()
    store.wait()


def after_kernel(pair, r1, r2, r3, mine, gain, info, after, sent):
    branch = pair[...].astype(F32)
    for r in (r1, r2, r3):
        branch = branch + r[...].astype(F32)
    a = norm(RESIDUAL_SCALE * mine[...].astype(F32) + branch, gain[...]).astype(BF)
    after[...] = a
    f = info[...]
    for j in range(8):
        sent[j, :, 0:2048] = a
        sent[j, :, 2048:2176] = f


def hidden_kernel(b0, b1, b3, near_half, far_half, w_all, side, h_out, pt_out, acts, info, xo, xp):
    for k, b in ((0, b0), (1, b1), (3, b3)):
        acts[64 * k : 64 * k + 64, :] = b[:, 0:2048]
        info[64 * k : 64 * k + 64, :] = b[:, 2048:2176].astype(F32)
    odd = lax.rem(lax.axis_index("y"), 2) * 32
    for start, b in ((128 + odd, near_half), (160 - odd, far_half)):
        here = pl.ds(pl.multiple_of(start, 32), 32)
        acts[here, :] = b[:, 0:2048]
        info[here, :] = b[:, 2048:2176].astype(F32)
    a = acts[...]
    lane = lax.broadcasted_iota(jnp.int32, (256, 128), 1)
    row = lax.broadcasted_iota(jnp.int32, (256, 128), 0)
    f = info[...]
    w = pltpu.roll(f, 128 - 8, 1) + pltpu.roll(f, 128 - 16, 1)
    zi = lax.axis_index("z")
    e0 = ((zi * 4 + lax.axis_index("x")) * 2).astype(F32)
    named = lane < 6
    m0 = jnp.logical_and(f == e0, named)
    m1 = jnp.logical_and(f == e0 + 1.0, named)
    s0 = jnp.sum(jnp.where(m0, w, 0.0), axis=1, keepdims=True)
    s1 = jnp.sum(jnp.where(m1, w, 0.0), axis=1, keepdims=True)
    a0 = jnp.sum(jnp.where(m0, 1.0, 0.0), axis=1, keepdims=True)
    a1 = jnp.sum(jnp.where(m1, 1.0, 0.0), axis=1, keepdims=True)
    flags = jnp.where(lane == 0, a0, jnp.where(lane == 1, a1, 0.0)).astype(BF)
    r2 = lax.broadcasted_iota(jnp.int32, (256, 256), 0)
    c2 = lax.broadcasted_iota(jnp.int32, (256, 256), 1)
    earlier = jnp.logical_and((r2 >> 3) == (c2 >> 3), c2 < r2)
    rank = dot(jnp.where(earlier, 1.0, 0.0).astype(BF), flags)
    base = ((row >> 3) * 2).astype(F32)
    lane_f = lane.astype(F32)
    t0 = jnp.logical_and(a0 > 0.5, base + rank[:, 0:1] == lane_f)
    t1 = jnp.logical_and(a1 > 0.5, base + rank[:, 1:2] == lane_f - 64.0)
    pt = jnp.where(jnp.where(lane < 64, jnp.where(t0, 1.0, 0.0), jnp.where(t1, 1.0, 0.0)) > 0.5, 1.0, 0.0)
    pt_out[...] = pt.astype(BF)
    pm = pt.T.astype(BF)

    switch = 1.0 / (1.0 + jnp.exp(-dot_nt(a, side[...])[:, 0:1]))
    share = jnp.where(lane < 64, s0, s1)

    def hidden_of(start, tail):
        gate = dot_nt(a, w_all[start : start + 256, :])
        up = dot_nt(a, w_all[start + 256 : start + 512, :])
        h = silu(gate) * up
        x = h[:, 128:256]
        tail[...] = x
        return (h[:, 0:128] * share).astype(BF), x * switch

    ho, do = hidden_of(0, xo)
    hp, dp = hidden_of(512, xp)
    eo = dot(pm, ho)
    ep = dot(pm, hp)
    lane1 = lane[:128]
    row1 = row[:128]
    near = lane1 < 64
    upper = jnp.where(near, eo, pltpu.roll(ep, 64, 1))
    lower = jnp.where(near, pltpu.roll(eo, 64, 1), ep)
    h_out[128:256, :] = jnp.where(row1 < 64, upper, lower).astype(BF)
    dense = jnp.where(lane < 32, do, pltpu.roll(dp, 32, 1))
    h_out[0:128, :] = jnp.where(near, dense[0:128], pltpu.roll(dense[128:256], 64, 1)).astype(BF)
    mine = pl.ds(pl.multiple_of(zi * 8, 8), 8)
    so, sp = xo[mine, :], xp[mine, :]
    s = jnp.where(lane[:8] < 64, pltpu.roll(so, 96, 1), pltpu.roll(sp, 32, 1))
    h_out[256:272, :] = jnp.concatenate([s, jnp.zeros((8, 128), F32)], axis=0).astype(BF)


def down_kernel(h0, h1, h2, h3, pt, d_all, out, shared):
    hs = (h0, h1, h2, h3)
    near = lax.broadcasted_iota(jnp.int32, (128, 128), 1) < 64
    total = None
    for n in range(2):
        u = hs[2 * n][0:128, :].astype(F32)
        v = hs[2 * n + 1][0:128, :].astype(F32)
        top = jnp.where(near, u, pltpu.roll(v, 64, 1))
        bottom = jnp.where(near, pltpu.roll(u, 64, 1), v)
        h = jnp.concatenate([top, bottom], axis=0).astype(BF)
        part = dot(h, d_all[1536 + 128 * n : 1664 + 128 * n, :])
        total = part if total is None else total + part
    outs = []
    for e in range(2):
        h = jnp.concatenate([r[128 + 64 * e : 192 + 64 * e, :] for r in hs], axis=1)
        outs.append(dot(h, d_all[512 * e : 512 * e + 512, :]))
    total = total + dot(pt[...], jnp.concatenate(outs, axis=0).astype(BF))
    h = jnp.concatenate([r[256:272, :] for r in hs], axis=1)
    shared[...] = dot(h, d_all[1024:1536, :])[0:8]
    for k in range(4):
        block = total[64 * k : 64 * k + 64].astype(BF).reshape(8, 8, 512)
        out[:, lax.rem(lax.axis_index("x") + 4 - k, 4)] = block


def sum_kernel(back, shared, out):
    total = shared[...]
    for j in range(32):
        total = total + back[j].astype(F32)
    out[...] = total


def both_kernel(own, other, out):
    first = lax.axis_index("c") == 0
    out[0:8] = jnp.where(first, own[...], other[...])
    out[8:16] = jnp.where(first, other[...], own[...])


def last_kernel(s0, s1, s2, s3, own, other, gain, out, whole):
    for k, s in enumerate((s0, s1, s2, s3)):
        start = lax.rem(lax.axis_index("y") + 4 - k, 4) * 512
        whole[:, pl.ds(pl.multiple_of(start, 512), 512)] = s[...]
    first = lax.axis_index("c") == 0
    a, b = own[...].astype(F32), other[...].astype(F32)
    rows = jnp.concatenate([jnp.where(first, a, b), jnp.where(first, b, a)], axis=0)
    out[...] = norm(RESIDUAL_SCALE * rows + whole[...], gain[...]).astype(BF)


def limit(mib):
    return pltpu.CompilerParams(vmem_limit_bytes=mib * 2**20)


def shape(*dims, dtype=BF):
    return pltpu.VMEM(dims, dtype)


def near(value):
    return pltpu.with_memory_space_constraint(value, pltpu.VMEM)


def big(value):
    return pltpu.with_memory_space_constraint(value, pltpu.HBM)


def layer(
    tokens,
    lengths,
    old_state,
    query_weight,
    key_weight,
    value_weight,
    gate_weight,
    head_gain,
    output_weight,
    first_gain,
    expert_ids,
    expert_weights,
    expert_gate,
    expert_up,
    expert_down,
    shared_gate,
    shared_up,
    shared_down,
    side_gate,
    dense_gate,
    dense_up,
    dense_down,
    second_gain,
):
    frequency = np.asarray(1.0 / 10000.0 ** ((np.arange(128) % 64) / 64.0), np.float32)
    state = old_state.reshape(16, 128, 128)
    outs = pl.pallas_call(
        mixer_kernel,
        in_specs=[HB] * 16,
        out_specs=[VM] * 11,
        out_shape=[shape(8, 2048)] * 2
        + [shape(16, 128, dtype=F32)] * 2
        + [shape(224, 512)] * 4
        + [shape(8, 2048), shape(8, 128), shape(1, 2048, dtype=F32)],
        scratch_shapes=[
            pltpu.SMEM((16,), jnp.int32),
            pltpu.VMEM((1, 128), F32),
            pltpu.VMEM((16, 2048), BF),
            pltpu.VMEM((1, 128), F32),
        ]
        + [pltpu.VMEM((2048, 128), BF)] * 4
        + [
            pltpu.VMEM((16, 128, 128), F32),
            pltpu.VMEM((128, 2048), BF),
            pltpu.VMEM((6, 16), jnp.int32),
            pltpu.VMEM((6, 16), F32),
            pltpu.VMEM((16, 128), F32),
            pltpu.VMEM((128, 128), F32),
            pltpu.SemaphoreType.DMA((13,)),
            pltpu.SemaphoreType.DMA((16,)),
        ],
        compiler_params=limit(8),
        name="mixer",
    )(
        *[
            big(v)
            for v in (
                lengths, jnp.asarray(frequency)[None], tokens, head_gain.reshape(1, 128),
                query_weight, key_weight, value_weight, gate_weight, state, output_weight,
                expert_down, dense_down, shared_down, expert_ids.T, expert_weights.T,
                first_gain.reshape(1, 2048),
            )
        ]
    )
    kept, given, keys, values = outs[0:4]
    downs, (mine, info, g1) = outs[4:8], outs[8:11]

    pair = (kept.astype(F32) + shifted(given, "c", 1).astype(F32)).astype(BF)
    raw = (
        expert_gate.transpose(0, 2, 1), expert_up.transpose(0, 2, 1),
        dense_gate.T, dense_up.T, shared_gate.T, shared_up.T,
    )
    side = jnp.broadcast_to(side_gate[None], (8, 2048))
    side, downs, raw, pair = lax.optimization_barrier((side, downs, raw, pair))
    arrived = [shifted(pair, "y", k) for k in range(1, 4)]
    peers = [shifted(r, "c", 1) for r in raw]
    from_y = [downs[0]] + [shifted(downs[k], "y", k) for k in range(1, 4)]
    after, sent = pl.pallas_call(
        after_kernel,
        in_specs=[VM] * 7,
        out_specs=[VM, VM],
        out_shape=[shape(8, 2048), shape(8, 8, 2176)],
        compiler_params=limit(4),
        name="after",
    )(pair, *arrived, mine, g1, info)

    side, sent = lax.optimization_barrier((side, sent))
    block = lax.all_to_all(sent, "z", 0, 0, tiled=True).reshape(64, 2176)
    other = shifted(after, "c", 1)
    part = lax.dynamic_slice_in_dim(block, (lax.axis_index("y") % 2) * 32, 32, 0)
    near_half = shifted(part, "x", 2)
    far_half = lax.ppermute(near_half, "y", [(0, 1), (1, 0), (2, 3), (3, 2)])
    blocks = [block] + [shifted(block, "x", k) for k in (1, 3)] + [near_half, far_half]
    from_c = [shifted(d, "c", 1) for d in from_y]
    w_all = pl.pallas_call(
        pack_kernel,
        in_specs=[HB] * 12,
        out_specs=VM,
        out_shape=shape(1024, 2048),
        scratch_shapes=[pltpu.SemaphoreType.DMA((20,))],
        compiler_params=limit(2),
        name="pack",
    )(*[big(v) for v in raw], *peers)
    new_state = pl.pallas_call(
        state_kernel,
        in_specs=[VM, VM, HB],
        out_specs=HB,
        out_shape=pltpu.HBM((16, 128, 128), F32),
        scratch_shapes=[
            pltpu.VMEM((16, 128, 128), F32),
            pltpu.VMEM((16, 128, 128), F32),
            pltpu.SemaphoreType.DMA((2,)),
        ],
        compiler_params=limit(4),
        name="state",
    )(keys, values, big(state))

    hidden, slots = pl.pallas_call(
        hidden_kernel,
        in_specs=[VM] * 7,
        out_specs=[VM] * 2,
        out_shape=[shape(272, 128), shape(256, 128)],
        scratch_shapes=[
            pltpu.VMEM((256, 2048), BF),
            pltpu.VMEM((256, 128), F32),
            pltpu.VMEM((256, 128), F32),
            pltpu.VMEM((256, 128), F32),
        ],
        compiler_params=limit(8),
        name="hidden",
    )(*blocks, near(w_all), side)
    h2, h1, h3 = (shifted(hidden, "y", k) for k in (2, 1, 3))
    gathered = [hidden, h1, h2, h3]
    d_all, g2 = pl.pallas_call(
        arrange_kernel,
        in_specs=[VM] * 8 + [HB],
        out_specs=[VM, VM],
        out_shape=[shape(1792, 512), shape(1, 2048, dtype=F32)],
        scratch_shapes=[pltpu.SemaphoreType.DMA((1,))],
        compiler_params=limit(2),
        name="arrange",
    )(*from_y, *from_c, big(second_gain.reshape(1, 2048)))
    partial, shared = pl.pallas_call(
        down_kernel,
        in_specs=[VM] * 6,
        out_specs=[VM, VM],
        out_shape=[shape(8, 4, 8, 512), shape(8, 512, dtype=F32)],
        compiler_params=limit(6),
        name="down",
    )(*gathered, slots, near(d_all))

    back = lax.all_to_all(partial.reshape(32, 8, 512), EP, 0, 0, tiled=True)
    total = pl.pallas_call(
        sum_kernel,
        in_specs=[VM, VM],
        out_specs=VM,
        out_shape=shape(8, 512, dtype=F32),
        compiler_params=limit(3),
        name="sum",
    )(back, shared)
    both = pl.pallas_call(
        both_kernel,
        in_specs=[VM] * 2,
        out_specs=VM,
        out_shape=shape(16, 512, dtype=F32),
        compiler_params=limit(3),
        name="both",
    )(total, shifted(total, "c", 1))
    s2, s1, s3 = (shifted(both, "y", k) for k in (2, 1, 3))
    layer_out = pl.pallas_call(
        last_kernel,
        in_specs=[VM] * 7,
        out_specs=VM,
        out_shape=jax.ShapeDtypeStruct((16, 2048), BF),
        scratch_shapes=[pltpu.VMEM((16, 2048), F32)],
        compiler_params=limit(3),
        name="last",
    )(both, s1, s2, s3, after, other, g2)
    return (layer_out, new_state.reshape(16, 1, 128, 128))


def solution(mesh):
    finer = Mesh(mesh.devices.reshape(8, 4, 4, 2), ALL)
    return jax.shard_map(
        layer,
        mesh=finer,
        in_specs=(
            P(EP, None),
            P(EP),
            P(EP, TP, None, None),
            P(None, TP),
            P(None, TP),
            P(None, TP),
            P(None, TP),
            P(TP),
            P(TP, None),
            P(),
            P(EP, None),
            P(EP, None),
            P(EP, None, TP),
            P(EP, None, TP),
            P(EP, TP, None),
            P(None, TP),
            P(None, TP),
            P(TP, None),
            P(),
            P(None, ALL),
            P(None, ALL),
            P(ALL, None),
            P(),
        ),
        out_specs=(P(EP, None), P(EP, TP, None, None)),
        check_vma=False,
    )
```
